512 devices in a mesh: sp: 128 (over z, x, core), tp: 4 (over y).
Axes of the slice: x: 4, y: 4, z: 16, core: 2. Of those that a mesh axis runs over, the one named last changes fastest.
Arguments:
- tokens: bfloat16 [16384, 1024], P(('sp', 'tp')), may hold values from -13 to 13, as said below
- norm_gain: float32 [1024], replicated, may hold values from 0.5 to 1.5
- query_weight: bfloat16 [1024, 4096], P(None, 'tp'), may hold values from -0.1875 to 0.1875
- key_weight: bfloat16 [1024, 512], P(None, 'tp'), may hold values from -0.1875 to 0.1875
- value_weight: bfloat16 [1024, 512], P(None, 'tp'), may hold values from -0.1875 to 0.1875
- query_gain: float32 [128], replicated, may hold values from 0.5 to 1.5
- key_gain: float32 [128], replicated, may hold values from 0.5 to 1.5
- output_weight: bfloat16 [4096, 1024], P('tp'), may hold values from -1 to 1
Outputs:
- mixed: bfloat16 [16384, 1024], P(('sp', 'tp'))
The draws below stay inside these ranges and needn't reach their ends.
Inputs may be any that keep to these rules, and one draw needn't show every extreme that they name: Every entry of tokens lies between -13 and 13.
All inputs are finite; a program needn't handle non-finite values.
Results may differ from the reference program's by a relative error of at most 0.015.
Values may be sent and summed in bfloat16 or wider, within the bound.
No kernel may reach another device: no remote copies, remote signals or barrier semaphores. Data moves between devices by JAX's collectives and lax.ppermute only.
A program may use at most 64 MiB of HBM per device.

```python
import jax
import jax.numpy as jnp
from jax import lax

D = 1024
HEADS = 32
KV_HEADS = 4
HEAD_DIM = 128
GRID_W = 64
TOK_SP = 128
TOKENS = 16384


def draw_tokens(key, part):
    noise_key = jax.random.fold_in(key, 11)
    region_key = jax.random.fold_in(key, 12)
    regions = TOKENS // TOK_SP
    noise_part = jnp.clip(jax.random.normal(noise_key, (TOKENS, D), jnp.float32), -4.0, 4.0)
    centres = 1.5 * jnp.clip(jax.random.normal(region_key, (regions, D), jnp.float32), -3.0, 3.0)
    spread_means = jnp.broadcast_to(centres[:, None, :], (regions, TOK_SP, D)).reshape(TOKENS, D)
    return (noise_part + spread_means).astype(jnp.bfloat16)


def shard_levels(stream_key, extent, cuts, smallest, largest):
    level = 1.0
    for dim, blocks in cuts:
        steps = jax.random.uniform(jax.random.fold_in(jax.random.fold_in(stream_key, 6), dim), (blocks,), jnp.float32, smallest / len(cuts), largest / len(cuts))
        level = level * jnp.repeat(jnp.exp(steps), extent[dim] // blocks).reshape((-1,) + (1,) * (len(extent) - 1 - dim))
    return level


def centred(key, extent, deviation, limit, shards=(), held_as=jnp.bfloat16):
    array = deviation * jax.random.normal(key, extent, jnp.float32)
    if shards:
        array = array * shard_levels(key, extent, shards, -0.22, 0.18)
    return jnp.clip(array, -limit, limit).astype(held_as)


def setup_inputs(seed: int = 0) -> dict:
    key_list = jax.random.split(jax.random.key(seed), 9)
    tokens = draw_tokens(jax.random.fold_in(key_list[8], 71), 0)
    norm_gain = jnp.clip(1.0 + 0.1 * jax.random.normal(key_list[1], (D,), jnp.float32), 0.5, 1.5)
    query_weight = centred(key_list[2], (D, HEADS * HEAD_DIM), D ** -0.5, 0.1875, ((1, 4),))
    key_weight = centred(key_list[3], (D, KV_HEADS * HEAD_DIM), D ** -0.5, 0.1875, ((1, 4),))
    value_weight = centred(key_list[4], (D, KV_HEADS * HEAD_DIM), D ** -0.5, 0.1875, ((1, 4),))
    query_gain = jnp.clip(1.0 + 0.1 * jax.random.normal(key_list[5], (HEAD_DIM,), jnp.float32), 0.5, 1.5)
    key_gain = jnp.clip(1.0 + 0.1 * jax.random.normal(key_list[6], (HEAD_DIM,), jnp.float32), 0.5, 1.5)
    output_weight = centred(key_list[7], (HEADS * HEAD_DIM, D), (HEADS * HEAD_DIM * TOK_SP // TOKENS) ** -0.5, 1.0, ((0, 4),))
    return dict(tokens=tokens, norm_gain=norm_gain, query_weight=query_weight, key_weight=key_weight, value_weight=value_weight, query_gain=query_gain, key_gain=key_gain, output_weight=output_weight)


epsilon = 1e-06
rotary_base = 10000.0

def rotation_tables(first_position, length, head_dim):
    positions = first_position + lax.iota(jnp.int32, length)
    grid_row = (positions // GRID_W).astype(jnp.float32)
    grid_column = (positions % GRID_W).astype(jnp.float32)
    axis_dim = head_dim // 2
    frequencies = rotary_base ** (-jnp.arange(0, axis_dim, 2, dtype=jnp.float32) / axis_dim)
    angles = jnp.concatenate([grid_row[:, None] * frequencies[None, :], grid_column[:, None] * frequencies[None, :]], axis=-1)
    return (jnp.cos(angles), jnp.sin(angles))

def normalize_rotate(projected, gain, cosine, sine):
    widened = projected.astype(jnp.float32)
    scaled = widened * lax.rsqrt(lax.optimization_barrier(jnp.mean(widened * widened, axis=-1, keepdims=True)) + epsilon) * gain.astype(jnp.float32)
    paired = scaled.reshape(scaled.shape[:-1] + (scaled.shape[-1] // 2, 2))
    even_half = paired[..., 0]
    odd_half = paired[..., 1]
    cosine_rows = cosine[:, None, :]
    sine_rows = sine[:, None, :]
    turned = jnp.stack([even_half * cosine_rows - odd_half * sine_rows, even_half * sine_rows + odd_half * cosine_rows], axis=-1)
    return turned.reshape(projected.shape).astype(jnp.bfloat16)

def rms_rows(tokens, norm_gain):
    widened = tokens.astype(jnp.float32)
    scaled = widened * lax.rsqrt(lax.optimization_barrier(jnp.mean(widened * widened, axis=-1, keepdims=True)) + epsilon)
    return (scaled * norm_gain.astype(jnp.float32)).astype(jnp.bfloat16)

def reference(tokens, norm_gain, query_weight, key_weight, value_weight, query_gain, key_gain, output_weight):
    normed = rms_rows(tokens, norm_gain)
    query_part = jnp.dot(normed, query_weight, preferred_element_type=jnp.float32).astype(jnp.bfloat16)
    key_part = jnp.dot(normed, key_weight, preferred_element_type=jnp.float32).astype(jnp.bfloat16)
    value_part = jnp.dot(normed, value_weight, preferred_element_type=jnp.float32).astype(jnp.bfloat16)
    cosine, sine = rotation_tables(0, TOKENS, HEAD_DIM)
    queries = normalize_rotate(query_part.reshape(TOKENS, HEADS, HEAD_DIM), query_gain, cosine, sine)
    keys = normalize_rotate(key_part.reshape(TOKENS, KV_HEADS, HEAD_DIM), key_gain, cosine, sine)
    key_all = keys.astype(jnp.float32)
    value_all = value_part.reshape(TOKENS, KV_HEADS, HEAD_DIM).astype(jnp.float32)
    group_size = HEADS // KV_HEADS
    block_count = TOKENS // GRID_W
    query_blocks = queries.reshape(block_count, GRID_W, KV_HEADS, group_size, HEAD_DIM)
    scale = HEAD_DIM ** (-0.5)

    def one_block(query_block):
        scores = jnp.einsum('qkgd,skd->kgqs', query_block.astype(jnp.float32), key_all, precision=lax.Precision.HIGHEST) * scale
        highest = lax.optimization_barrier(jnp.max(scores, axis=-1, keepdims=True))
        weights = jnp.exp(scores - highest)
        denominator = lax.optimization_barrier(jnp.sum(weights, axis=-1))
        rounded = lax.optimization_barrier(weights.astype(jnp.bfloat16)).astype(jnp.float32)
        numerator = jnp.einsum('kgqs,skd->kgqd', rounded, value_all, precision=lax.Precision.HIGHEST)
        return (numerator / denominator[..., None]).astype(jnp.bfloat16)
    attended = lax.map(one_block, query_blocks)
    attended = attended.transpose(0, 3, 1, 2, 4).reshape(TOKENS, HEADS * HEAD_DIM)
    return jnp.dot(attended, output_weight, preferred_element_type=jnp.float32).astype(jnp.bfloat16)
```

```python
import math

import jax
import jax.numpy as jnp
import numpy as np
from jax import lax
from jax.experimental import pallas as pl
from jax.experimental.pallas import tpu as pltpu
from jax.sharding import Mesh, PartitionSpec as P

GRID_W = 64
EPS = 1e-06
BASE = 10000.0
HD = 128
TOK = 128
NZ, NX, NC, NY = 16, 4, 2, 4
LROWS = 8
AROWS = HD + LROWS
PROWS = HD + 2 * LROWS
CHUNK = 512


def rotary_tables(grid_rows):
    axis_dim = HD // 2
    freq = np.power(np.float32(BASE), -np.arange(0, axis_dim, 2, dtype=np.float32) / np.float32(axis_dim))
    sign = np.tile(np.array([-1.0, 1.0]), axis_dim // 2)

    def half(count):
        angle = (np.arange(count, dtype=np.float32)[:, None] * freq[None, :].astype(np.float32)).astype(np.float64)
        angle = np.repeat(angle, 2, axis=1)
        return np.cos(angle), np.sin(angle) * sign

    row_cos, row_sin = half(grid_rows)
    col_cos, col_sin = half(GRID_W)
    pad_r, pad_c = np.ones_like(row_cos), np.ones_like(col_cos)
    rows = np.stack([np.concatenate([row_cos, pad_r], 1), np.concatenate([row_sin, pad_r], 1)])
    cols = np.stack([np.concatenate([pad_c, col_cos], 1), np.concatenate([pad_c, col_sin], 1)])
    return rows.astype(np.float32), cols.astype(np.float32)


VM = pl.BlockSpec(memory_space=pltpu.VMEM)


def call(kernel, shapes, name, *args, smem=0, flops=0, limit=24, alias=None):
    return pl.pallas_call(
        kernel,
        out_shape=shapes,
        in_specs=[pl.BlockSpec(memory_space=pltpu.SMEM)] * smem + [VM] * (len(args) - smem),
        out_specs=jax.tree.map(lambda s: VM, shapes),
        name=name,
        input_output_aliases=alias or {},
        cost_estimate=pl.CostEstimate(flops=flops, bytes_accessed=1 << 20, transcendentals=0),
        compiler_params=pltpu.CompilerParams(vmem_limit_bytes=limit << 20),
    )(*args)


def bf16(*shape):
    return jax.ShapeDtypeStruct(shape, jnp.bfloat16)


def f32(*shape):
    return jax.ShapeDtypeStruct(shape, jnp.float32)


def project_kernel(sp_ref, tok_ref, ng_ref, wq_ref, wk_ref, wv_ref, qg_ref, kg_ref, rows_ref, cols_ref, q_ref, kv_ref):
    x = tok_ref[...].astype(jnp.float32)
    normed = x * lax.rsqrt(jnp.mean(x * x, axis=-1, keepdims=True) + EPS) * ng_ref[...]
    normed = normed.astype(jnp.bfloat16)
    first = sp_ref[0] * (TOK // GRID_W)

    def table(i):
        parts = [rows_ref[i, pl.ds(first + r, 1), :] * cols_ref[i] for r in range(TOK // GRID_W)]
        return jnp.concatenate(parts, axis=0)

    cosine, sine = table(0), table(1)
    even = lax.broadcasted_iota(jnp.int32, (TOK, HD), 1) % 2 == 0

    def turn(projected, gain):
        wide = projected.astype(jnp.bfloat16).astype(jnp.float32)
        wide = wide * lax.rsqrt(jnp.mean(wide * wide, axis=-1, keepdims=True) + EPS) * gain
        swapped = jnp.where(even, pltpu.roll(wide, HD - 1, 1), pltpu.roll(wide, 1, 1))
        return wide * cosine + swapped * sine

    keys = jnp.dot(normed, wk_ref[...], preferred_element_type=jnp.float32)
    kv_ref[0] = turn(keys, kg_ref[...]).astype(jnp.bfloat16)
    values = jnp.dot(normed, wv_ref[...], preferred_element_type=jnp.float32)
    kv_ref[1] = values.T.astype(jnp.bfloat16)
    queries = jnp.dot(normed, wq_ref[...], preferred_element_type=jnp.float32)
    fold = HD ** (-0.5) * math.log2(math.e)
    for h in range(queries.shape[1] // HD):
        turned = turn(queries[:, h * HD : (h + 1) * HD], qg_ref[...]) * fold
        q_ref[:, h * TOK : (h + 1) * TOK] = turned.T.astype(jnp.bfloat16)


def pack(total):
    below = total[HD:]
    high = below.astype(jnp.bfloat16)
    low = (below - high.astype(jnp.float32)).astype(jnp.bfloat16)
    return jnp.concatenate([total[:HD].astype(jnp.bfloat16), high, low], axis=0)


def unpack(packed):
    wide = packed.astype(jnp.float32)
    return jnp.concatenate([wide[:HD], wide[HD:AROWS] + wide[AROWS:]], axis=0)


def fold_kernel(nq, nkv, has_acc, packed, *refs):
    q_refs, kv_refs, out_ref = refs[:nq], refs[nq : nq + nkv], refs[-1]
    acc_ref = refs[nq + nkv] if has_acc else None
    blocks = [(kv, i) for kv in kv_refs for i in range(kv.shape[0])]
    ones = jnp.ones((LROWS, CHUNK), jnp.bfloat16)
    per = CHUNK // TOK
    keys, values = [], []
    for j in range(0, len(blocks), per):
        group = blocks[j : j + per]
        keys.append(jnp.concatenate([kv[i, 0] for kv, i in group], axis=0))
        columns = jnp.concatenate([kv[i, 1] for kv, i in group], axis=1)
        values.append(jnp.concatenate([columns, ones], axis=0))
    for t in range(nq):
        q = q_refs[t][...]
        total = acc_ref[t] if has_acc else None
        for k, v in zip(keys, values):
            weights = jnp.exp2(jnp.dot(k, q, preferred_element_type=jnp.float32)).astype(jnp.bfloat16)
            part = jnp.dot(v, weights, preferred_element_type=jnp.float32)
            total = part if total is None else total + part
        out_ref[t] = pack(total) if packed else total


def fold(queries, blocks, acc, packed=False):
    nq, rows = len(queries), queries[0].shape[1]
    keys = sum(b.shape[0] for b in blocks) * TOK
    shape = bf16(nq, PROWS, rows) if packed else f32(nq, AROWS, rows)

    def kernel(*refs):
        fold_kernel(nq, len(blocks), acc is not None, packed, *refs)

    args = tuple(queries) + tuple(blocks) + (() if acc is None else (acc,))
    alias = {} if acc is None or packed else {len(args) - 1: 0}
    return call(kernel, shape, "fold", *args, flops=4 * nq * rows * keys * HD, alias=alias)


def merge_kernel(acc_ref, other_ref, own_ref, *out_refs):
    own_ref[...] = acc_ref[0] + unpack(other_ref[0])
    for t, out_ref in enumerate(out_refs):
        out_ref[...] = pack(acc_ref[t + 1] + unpack(other_ref[t + 1]))


def finish_kernel(own_ref, a_ref, b_ref, d_ref, w_ref, out_ref):
    total = own_ref[...] + unpack(a_ref[...]) + unpack(b_ref[...]) + unpack(d_ref[...])
    quotient = total[:HD] * (1.0 / total[HD : HD + 1])
    heads = [quotient[:, i : i + TOK].T.astype(jnp.bfloat16) for i in range(0, quotient.shape[1], TOK)]
    attended = jnp.concatenate(heads, axis=1)
    out_ref[...] = jnp.dot(attended, w_ref[...], preferred_element_type=jnp.float32).astype(jnp.bfloat16)


def sum_kernel(part_ref, out_ref):
    total = part_ref[0].astype(jnp.float32)
    for p in range(1, part_ref.shape[0]):
        total = total + part_ref[p].astype(jnp.float32)
    out_ref[...] = total.astype(out_ref.dtype)


def shift(array, axis, size, by):
    return lax.ppermute(array, axis, [(i, (i + by) % size) for i in range(size)])


def per_device(tables, tokens, norm_gain, wq, wk, wv, query_gain, key_gain, wo):
    z, x, c = (lax.axis_index(a) for a in ("z", "x", "c"))
    sp = (z * NX + x) * NC + c
    rows = tokens.shape[0]
    width = wq.shape[1]
    copies = jnp.broadcast_to(tokens[None], (NY,) + tokens.shape)
    mine = lax.all_to_all(copies, "y", 0, 0, tiled=True).reshape(NY * rows, -1)
    q, kv = call(
        project_kernel,
        (bf16(HD, width), bf16(2, TOK, HD)),
        "project",
        jnp.reshape(sp, (1,)).astype(jnp.int32),
        mine,
        norm_gain.reshape(1, -1),
        wq,
        wk,
        wv,
        query_gain.reshape(1, -1),
        key_gain.reshape(1, -1),
        *tables,
        smem=1,
        flops=2 * TOK * 1024 * 1280,
    )
    kv = kv[None]

    far = [kv] + [shift(kv, "z", NZ, by) for by in (4, -4, 8)]
    mine_q = [q] + [shift(q, "x", NX, by) for by in (1, -1, 2)]
    stack_q = jnp.stack(mine_q)
    group = jnp.concatenate(far, axis=0)
    near = [shift(group, "z", NZ, 1), shift(group, "z", NZ, -1)]
    both = [(i * NC, (i + 2) % NZ * NC) for i in range(NZ)] + [(i * NC + 1, (i - 2) % NZ * NC + 1) for i in range(NZ)]
    near.append(lax.ppermute(group, ("z", "c"), both))
    other_stack = shift(stack_q, "c", NC, 1)
    other_q = [other_stack[t] for t in range(NX)]

    own = fold(mine_q, [group], None)
    other = fold(other_q, [group], None)
    for block in near[:-1]:
        other = fold(other_q, [block], other)
        own = fold(mine_q, [block], own)
    other = fold(other_q, near[-1:], other, packed=True)
    arrived = shift(other, "c", NC, 1)
    own = fold(mine_q, near[-1:], own)
    kept, *sent = call(merge_kernel, (f32(AROWS, width),) + (bf16(PROWS, width),) * 3, "merge", own, arrived)
    back = [shift(s, "x", NX, by) for s, by in zip(sent, (-1, 1, 2))]
    mixed = call(finish_kernel, bf16(TOK, wo.shape[1]), "finish", kept, *back, wo, flops=2 * TOK * 1024 * 1024)
    shares = lax.all_to_all(mixed.reshape(NY, rows, -1), "y", 0, 0, tiled=True)
    return call(sum_kernel, bf16(*tokens.shape), "sum", shares)


def solution(mesh):
    fine = Mesh(mesh.devices.reshape(NZ, NX, NC, NY), ("z", "x", "c", "y"))
    sp = ("z", "x", "c")
    tables = rotary_tables(NZ * NX * NC * TOK // GRID_W)

    def run(*args):
        return per_device(tables, *args)

    return jax.shard_map(
        run,
        mesh=fine,
        in_specs=(
            P(sp + ("y",), None),
            P(),
            P(None, "y"),
            P(None, "y"),
            P(None, "y"),
            P(),
            P(),
            P("y", None),
        ),
        out_specs=P(sp + ("y",), None),
        check_vma=False,
    )
```

```python
import math

import jax
import jax.numpy as jnp
import numpy as np
from jax import lax
from jax.experimental import pallas as pl
from jax.experimental.pallas import tpu as pltpu
from jax.sharding import Mesh, PartitionSpec as P


GRID_W = 64
EPS = 1e-06
BASE = 10000.0
HD = 128
TOK = 128
NZ, NX, NC, NY = 16, 4, 2, 4
KEY_SCALE, VALUE_SCALE = 2.0**11, 2.0**7
LROWS = 8
AROWS = HD + LROWS
PROWS = HD + 2 * LROWS
CHUNK = 512


def rotary_tables(grid_rows):
    axis_dim = HD // 2
    freq = np.power(np.float32(BASE), -np.arange(0, axis_dim, 2, dtype=np.float32) / np.float32(axis_dim))
    sign = np.tile(np.array([-1.0, 1.0]), axis_dim // 2)

    def half(count):
        angle = (np.arange(count, dtype=np.float32)[:, None] * freq[None, :].astype(np.float32)).astype(np.float64)
        angle = np.repeat(angle, 2, axis=1)
        return np.cos(angle), np.sin(angle) * sign

    row_cos, row_sin = half(grid_rows)
    col_cos, col_sin = half(GRID_W)
    pad_r, pad_c = np.ones_like(row_cos), np.ones_like(col_cos)
    rows = np.stack([np.concatenate([row_cos, pad_r], 1), np.concatenate([row_sin, pad_r], 1)])
    cols = np.stack([np.concatenate([pad_c, col_cos], 1), np.concatenate([pad_c, col_sin], 1)])
    return rows.astype(np.float32), cols.astype(np.float32)


VM = pl.BlockSpec(memory_space=pltpu.VMEM)


def call(kernel, shapes, *args, smem=0, flops=0, limit=24, alias=None):
    return pl.pallas_call(
        kernel,
        out_shape=shapes,
        in_specs=[pl.BlockSpec(memory_space=pltpu.SMEM)] * smem + [VM] * (len(args) - smem),
        out_specs=jax.tree.map(lambda s: VM, shapes),
        input_output_aliases=alias or {},
        cost_estimate=pl.CostEstimate(flops=flops, bytes_accessed=1 << 20, transcendentals=0),
        compiler_params=pltpu.CompilerParams(vmem_limit_bytes=limit << 20),
    )(*args)


def bf16(*shape):
    return jax.ShapeDtypeStruct(shape, jnp.bfloat16)


def f32(*shape):
    return jax.ShapeDtypeStruct(shape, jnp.float32)


def spread_kernel(tok_ref, out_ref, sems):
    copies = [pltpu.make_async_copy(tok_ref, out_ref.at[i], sems.at[i]) for i in range(NY)]
    for copy in copies:
        copy.start()
    for copy in copies:
        copy.wait()


def to_vmem(kernel, shapes, *args, count, limit=60):
    return pl.pallas_call(
        kernel,
        out_shape=shapes,
        in_specs=[pl.BlockSpec(memory_space=pltpu.HBM)] * len(args),
        out_specs=jax.tree.map(lambda s: VM, shapes),
        scratch_shapes=[pltpu.SemaphoreType.DMA((count,))],
        cost_estimate=pl.CostEstimate(flops=1 << 28, bytes_accessed=1 << 20, transcendentals=0),
        compiler_params=pltpu.CompilerParams(vmem_limit_bytes=limit << 20),
    )(*args)


def project_kernel(sp_ref, tok_ref, w_ref, vec_ref, rows_ref, cols_ref, q_ref, kv_ref):
    x = tok_ref[...].astype(jnp.float32)
    dim = x.shape[1]
    wide_q = w_ref.shape[1] - 2 * HD
    query_gain, key_gain = vec_ref[:, dim : dim + HD], vec_ref[:, dim + HD :]
    normed = x * lax.rsqrt(jnp.mean(x * x, axis=-1, keepdims=True) + EPS) * vec_ref[:, :dim]
    normed = normed.astype(jnp.bfloat16)
    first = sp_ref[0] * (TOK // GRID_W)

    def table(i):
        parts = [rows_ref[i, pl.ds(first + r, 1), :] * cols_ref[i] for r in range(TOK // GRID_W)]
        return jnp.concatenate(parts, axis=0)

    cosine, sine = table(0), table(1)
    even = lax.broadcasted_iota(jnp.int32, (TOK, HD), 1) % 2 == 0

    def turn(projected, gain):
        wide = projected.astype(jnp.bfloat16).astype(jnp.float32)
        wide = wide * lax.rsqrt(jnp.mean(wide * wide, axis=-1, keepdims=True) + EPS) * gain
        swapped = jnp.where(even, pltpu.roll(wide, HD - 1, 1), pltpu.roll(wide, 1, 1))
        return wide * cosine + swapped * sine

    keys = jnp.dot(normed, w_ref[:, wide_q : wide_q + HD], preferred_element_type=jnp.float32)
    keys = turn(keys, key_gain).astype(jnp.bfloat16)
    values = jnp.dot(normed, w_ref[:, wide_q + HD :], preferred_element_type=jnp.float32).T.astype(jnp.bfloat16)
    kv_ref[0] = keys
    kv_ref[1] = values
    queries = jnp.dot(normed, w_ref[:, :wide_q], preferred_element_type=jnp.float32)
    fold = HD ** (-0.5) * math.log2(math.e) / KEY_SCALE
    for h in range(queries.shape[1] // HD):
        turned = turn(queries[:, h * HD : (h + 1) * HD], query_gain) * fold
        turned = turned.T.astype(jnp.bfloat16)
        for i in range(NX):
            q_ref[i, :, h * TOK : (h + 1) * TOK] = turned


def pack(total):
    below = total[HD:]
    high = below.astype(jnp.bfloat16)
    low = (below - high.astype(jnp.float32)).astype(jnp.bfloat16)
    return jnp.concatenate([total[:HD].astype(jnp.bfloat16), high, low], axis=0)


def unpack(packed):
    wide = packed.astype(jnp.float32)
    return jnp.concatenate([wide[:HD], wide[HD:AROWS] + wide[AROWS:]], axis=0)


def fold_kernel(start, count, first, packed, q_ref, kv_ref, *refs):
    out_ref = refs[-1]
    ones = jnp.full((LROWS, CHUNK), VALUE_SCALE, jnp.bfloat16)
    per = CHUNK // TOK
    keys, values = [], []
    for j in range(start, start + count, per):
        keys.append(jnp.concatenate([kv_ref[i, 0] for i in range(j, j + per)], axis=0))
        columns = jnp.concatenate([kv_ref[i, 1] for i in range(j, j + per)], axis=1)
        values.append(jnp.concatenate([columns, ones], axis=0))
    for t in range(q_ref.shape[0]):
        q = q_ref[t]
        total = None if first else refs[0][t]
        for k, v in zip(keys, values):
            weights = jnp.exp2(jnp.dot(k, q, preferred_element_type=jnp.float32)).astype(jnp.bfloat16)
            part = jnp.dot(v, weights, preferred_element_type=jnp.float32)
            total = part if total is None else total + part
        out_ref[t] = pack(total) if packed else total


def fold(queries, blocks, start, count, acc, packed=False):
    nq, _, rows = queries.shape
    shape = bf16(nq, PROWS, rows) if packed else f32(nq, AROWS, rows)

    def kernel(*refs):
        fold_kernel(start, count, acc is None, packed, *refs)

    args = (queries, blocks) + (() if acc is None else (acc,))
    alias = {} if acc is None or packed else {2: 0}
    return call(kernel, shape, *args, flops=4 * nq * rows * count * TOK * HD, alias=alias)


def merge_kernel(acc_ref, other_ref, out_ref):
    for t in range(acc_ref.shape[0]):
        out_ref[t] = pack(acc_ref[t] + unpack(other_ref[t]))


def finish_kernel(part_ref, w_ref, out_ref):
    total = unpack(part_ref[0])
    for t in range(1, part_ref.shape[0]):
        total = total + unpack(part_ref[t])
    quotient = total[:HD] * (1.0 / total[HD : HD + 1])
    heads = [quotient[:, i : i + TOK].T.astype(jnp.bfloat16) for i in range(0, quotient.shape[1], TOK)]
    attended = jnp.concatenate(heads, axis=1)
    out_ref[...] = jnp.dot(attended, w_ref[...], preferred_element_type=jnp.float32).astype(jnp.bfloat16)


def sum_kernel(part_ref, out_ref):
    total = part_ref[0].astype(jnp.float32)
    for p in range(1, part_ref.shape[0]):
        total = total + part_ref[p].astype(jnp.float32)
    out_ref[...] = total.astype(out_ref.dtype)


def per_device(tables, tokens, norm_gain, wq, wk, wv, query_gain, key_gain, wo):
    z, x, c = (lax.axis_index(a) for a in ("z", "x", "c"))
    sp = (z * NX + x) * NC + c
    rows, dim = tokens.shape
    width = wq.shape[1]
    copies = to_vmem(spread_kernel, bf16(NY, rows, dim), tokens, count=NY)
    mine = lax.all_to_all(copies, "y", 0, 0, tiled=True).reshape(NY * rows, dim)
    weights = jnp.concatenate([wq, wk, wv], axis=1)
    gains = jnp.concatenate([norm_gain, query_gain, key_gain]).reshape(1, -1)
    q, kv = call(
        project_kernel,
        (bf16(NX, HD, width), bf16(2, TOK, HD)),
        jnp.reshape(sp, (1,)).astype(jnp.int32),
        mine,
        weights,
        gains,
        *tables,
        smem=1,
        flops=2 * TOK * 1024 * 1280,
    )
    own_q = lax.all_to_all(q, "x", 0, 0, tiled=True)
    scaled = jnp.concatenate([kv[:1] * KEY_SCALE, kv[1:] * VALUE_SCALE]).astype(jnp.float16)
    gathered = lax.all_gather(scaled[None], "z", axis=0, tiled=True)
    other_q = lax.ppermute(own_q, "c", [(0, 1), (1, 0)])
    blocks = gathered.astype(jnp.bfloat16)
    half = NZ // 2
    own = fold(own_q, blocks, 0, half, None)
    other = fold(other_q, blocks, 0, half, None)
    other = fold(other_q, blocks, half, half, other, packed=True)
    arrived = lax.ppermute(other, "c", [(0, 1), (1, 0)])
    own = fold(own_q, blocks, half, half, own)
    merged = call(merge_kernel, bf16(NX, PROWS, width), own, arrived)
    parts = lax.all_to_all(merged, "x", 0, 0, tiled=True)
    mixed = call(finish_kernel, bf16(TOK, wo.shape[1]), parts, wo, flops=2 * TOK * 1024 * 1024)
    shares = lax.all_to_all(mixed.reshape(NY, rows, -1), "y", 0, 0, tiled=True)
    return call(sum_kernel, bf16(rows, dim), shares)


def solution(mesh):
    fine = Mesh(mesh.devices.reshape(NZ, NX, NC, NY), ("z", "x", "c", "y"))
    sp = ("z", "x", "c")
    tables = rotary_tables(NZ * NX * NC * TOK // GRID_W)

    def run(*args):
        return per_device(tables, *args)

    return jax.shard_map(
        run,
        mesh=fine,
        in_specs=(
            P(sp + ("y",), None),
            P(),
            P(None, "y"),
            P(None, "y"),
            P(None, "y"),
            P(),
            P(),
            P("y", None),
        ),
        out_specs=P(sp + ("y",), None),
        check_vma=False,
    )
```

```python
import math

import jax
import jax.numpy as jnp
import numpy as np
from jax import lax
from jax.experimental import pallas as pl
from jax.experimental.pallas import tpu as pltpu
from jax.sharding import Mesh, PartitionSpec as P


GRID_W = 64
EPS = 1e-06
BASE = 10000.0
HD = 128
TOK = 128
NZ, NX, NC, NY = 16, 4, 2, 4
KEY_SCALE, VALUE_SCALE = 2.0**11, 2.0**7
LROWS = 8
AROWS = HD + LROWS
PROWS = HD + LROWS
RINGS = [[i * NC + (i + g) % NC for i in range(NZ)] for g in range(NC)]
CHUNK = 512


def rotary_tables(grid_rows):
    axis_dim = HD // 2
    freq = np.power(np.float32(BASE), -np.arange(0, axis_dim, 2, dtype=np.float32) / np.float32(axis_dim))
    sign = np.tile(np.array([-1.0, 1.0]), axis_dim // 2)

    def half(count):
        angle = (np.arange(count, dtype=np.float32)[:, None] * freq[None, :].astype(np.float32)).astype(np.float64)
        angle = np.repeat(angle, 2, axis=1)
        return np.cos(angle), np.sin(angle) * sign

    row_cos, row_sin = half(grid_rows)
    col_cos, col_sin = half(GRID_W)
    pad_r, pad_c = np.ones_like(row_cos), np.ones_like(col_cos)
    rows = np.stack([np.concatenate([row_cos, pad_r], 1), np.concatenate([row_sin, pad_r], 1)])
    cols = np.stack([np.concatenate([pad_c, col_cos], 1), np.concatenate([pad_c, col_sin], 1)])
    return rows.astype(np.float32), cols.astype(np.float32)


VM = pl.BlockSpec(memory_space=pltpu.VMEM)


def call(kernel, shapes, *args, smem=0, flops=0, limit=24, alias=None):
    return pl.pallas_call(
        kernel,
        out_shape=shapes,
        in_specs=[pl.BlockSpec(memory_space=pltpu.SMEM)] * smem + [VM] * (len(args) - smem),
        out_specs=jax.tree.map(lambda s: VM, shapes),
        input_output_aliases=alias or {},
        cost_estimate=pl.CostEstimate(flops=flops, bytes_accessed=1 << 20, transcendentals=0),
        compiler_params=pltpu.CompilerParams(vmem_limit_bytes=limit << 20),
    )(*args)


def bf16(*shape):
    return jax.ShapeDtypeStruct(shape, jnp.bfloat16)


def f32(*shape):
    return jax.ShapeDtypeStruct(shape, jnp.float32)


def spread_kernel(tok_ref, out_ref, sems):
    copies = [pltpu.make_async_copy(tok_ref, out_ref.at[i], sems.at[i]) for i in range(NY)]
    for copy in copies:
        copy.start()
    for copy in copies:
        copy.wait()


def spread(array, count):
    return pl.pallas_call(
        spread_kernel,
        out_shape=jax.ShapeDtypeStruct((count,) + array.shape, array.dtype),
        in_specs=[VM],
        out_specs=pl.BlockSpec(memory_space=pltpu.HBM),
        scratch_shapes=[pltpu.SemaphoreType.DMA((count,))],
        name="spread",
    )(array)


def project_kernel(sp_ref, tok_ref, w_ref, vec_ref, rows_ref, cols_ref, q_ref, kv_ref, turned_ref, sems):
    x = tok_ref[...].astype(jnp.float32)
    dim = x.shape[1]
    wide_q = w_ref.shape[1] - 2 * HD
    query_gain, key_gain = vec_ref[:, dim : dim + HD], vec_ref[:, dim + HD :]
    normed = x * lax.rsqrt(jnp.mean(x * x, axis=-1, keepdims=True) + EPS) * vec_ref[:, :dim]
    normed = normed.astype(jnp.bfloat16)
    first = sp_ref[0] * (TOK // GRID_W)

    def table(i):
        parts = [rows_ref[i, pl.ds(first + r, 1), :] * cols_ref[i] for r in range(TOK // GRID_W)]
        return jnp.concatenate(parts, axis=0)

    cosine, sine = table(0), table(1)
    even = lax.broadcasted_iota(jnp.int32, (TOK, HD), 1) % 2 == 0

    def turn(projected, gain):
        wide = projected.astype(jnp.bfloat16).astype(jnp.float32)
        wide = wide * lax.rsqrt(jnp.mean(wide * wide, axis=-1, keepdims=True) + EPS) * gain
        swapped = jnp.where(even, pltpu.roll(wide, HD - 1, 1), pltpu.roll(wide, 1, 1))
        return wide * cosine + swapped * sine

    keys = jnp.dot(normed, w_ref[:, wide_q : wide_q + HD], preferred_element_type=jnp.float32)
    keys = turn(keys, key_gain).astype(jnp.bfloat16) * KEY_SCALE
    values = jnp.dot(normed, w_ref[:, wide_q + HD :], preferred_element_type=jnp.float32).T.astype(jnp.bfloat16) * VALUE_SCALE
    kv_ref[0] = keys
    kv_ref[1] = values
    queries = jnp.dot(normed, w_ref[:, :wide_q], preferred_element_type=jnp.float32)
    fold = HD ** (-0.5) * math.log2(math.e) / KEY_SCALE
    for h in range(queries.shape[1] // HD):
        turned = turn(queries[:, h * HD : (h + 1) * HD], query_gain) * fold
        turned_ref[:, h * TOK : (h + 1) * TOK] = turned.T.astype(jnp.bfloat16)
    copies = [pltpu.make_async_copy(turned_ref, q_ref.at[i], sems.at[i]) for i in range(NX)]
    for copy in copies:
        copy.start()
    for copy in copies:
        copy.wait()


def pack(total):
    below = total[HD:]
    high = below.astype(jnp.bfloat16).astype(jnp.float32)
    odd = lax.broadcasted_iota(jnp.int32, below.shape, 0) % 2 == 1
    return jnp.concatenate([total[:HD], jnp.where(odd, below - high, high)], axis=0).astype(jnp.bfloat16)


def unpack(packed):
    wide = packed.astype(jnp.float32)
    return jnp.concatenate([wide[:HD], wide[HD : HD + 1] + wide[HD + 1 : HD + 2]], axis=0)


def fold_kernel(tiles, sets, resumed, packed, at_ref, q_ref, *refs):
    kv_refs, sum_refs, out_refs = refs[:sets], refs[sets : len(refs) - tiles], refs[len(refs) - tiles :]
    ones = jnp.full((LROWS, CHUNK), VALUE_SCALE, jnp.bfloat16)
    per = CHUNK // TOK
    keys, values = [], []
    for kv_ref in kv_refs:
        for j in range(0, kv_ref.shape[0], per):
            keys.append(jnp.concatenate([kv_ref[i, 0] for i in range(j, j + per)], axis=0))
            columns = jnp.concatenate([kv_ref[i, 1] for i in range(j, j + per)], axis=1)
            values.append(jnp.concatenate([columns, ones], axis=0))
    for t in range(tiles):
        q = q_ref[at_ref[t]]
        total = sum_refs[t][...] if resumed else None
        for k, v in zip(keys, values):
            weights = jnp.exp2(jnp.dot(k, q, preferred_element_type=jnp.float32)).astype(jnp.bfloat16)
            part = jnp.dot(v, weights, preferred_element_type=jnp.float32)
            total = part if total is None else total + part
        out_refs[t][...] = pack(total) if packed else total


def fold(at, queries, blocks, sums=(), packed=False):
    tiles = at.shape[0]
    width = queries.shape[2]
    shape = tuple(bf16(PROWS, width) if packed else f32(AROWS, width) for _ in range(tiles))

    def kernel(*refs):
        fold_kernel(tiles, len(blocks), len(sums) > 0, packed, *refs)

    flops = 4 * tiles * width * sum(b.shape[0] for b in blocks) * TOK * HD
    return call(kernel, shape, at, queries, *blocks, *sums, smem=1, flops=flops)


def finish_kernel(own_ref, *refs):
    part_refs, w_ref, out_ref = refs[:-2], refs[-2], refs[-1]
    total = own_ref[: HD + 1]
    for part_ref in part_refs:
        total = total + unpack(part_ref[...])
    quotient = total[:HD] * (1.0 / total[HD : HD + 1])
    heads = [quotient[:, i : i + TOK].T.astype(jnp.bfloat16) for i in range(0, quotient.shape[1], TOK)]
    attended = jnp.concatenate(heads, axis=1)
    out_ref[...] = jnp.dot(attended, w_ref[...], preferred_element_type=jnp.float32).astype(jnp.bfloat16)


def sum_kernel(part_ref, out_ref):
    total = part_ref[0].astype(jnp.float32)
    for p in range(1, part_ref.shape[0]):
        total = total + part_ref[p].astype(jnp.float32)
    out_ref[...] = total.astype(out_ref.dtype)


def per_device(tables, tokens, norm_gain, wq, wk, wv, query_gain, key_gain, wo):
    z, x, c = (lax.axis_index(a) for a in ("z", "x", "c"))
    sp = (z * NX + x) * NC + c
    rows, dim = tokens.shape
    width = wq.shape[1]
    copies = spread(tokens, NY)
    mine = lax.all_to_all(copies, "y", 0, 0, tiled=True).reshape(NY * rows, dim)
    weights = jnp.concatenate([wq, wk, wv], axis=1)
    gains = jnp.concatenate([norm_gain, query_gain, key_gain]).reshape(1, -1)
    q, kv = pl.pallas_call(
        project_kernel,
        out_shape=(bf16(NX, HD, width), bf16(2, TOK, HD)),
        in_specs=[pl.BlockSpec(memory_space=pltpu.SMEM)] + [VM] * 5,
        out_specs=(pl.BlockSpec(memory_space=pltpu.HBM), VM),
        scratch_shapes=[pltpu.VMEM((HD, width), jnp.bfloat16), pltpu.SemaphoreType.DMA((NX,))],
        name="project",
        cost_estimate=pl.CostEstimate(flops=2 * TOK * dim * (width + 2 * HD), bytes_accessed=1 << 20, transcendentals=0),
        compiler_params=pltpu.CompilerParams(vmem_limit_bytes=24 << 20),
    )(jnp.reshape(sp, (1,)).astype(jnp.int32), mine, weights, gains, *tables)
    own_q = lax.all_to_all(q, "x", 0, 0, tiled=True)
    scaled = kv.astype(jnp.float16)
    gathered = lax.all_gather(scaled[None], ("z", "c"), axis_index_groups=RINGS, axis=0, tiled=True)
    blocks = gathered.astype(jnp.bfloat16)
    others = lax.ppermute(blocks, "c", [(0, 1), (1, 0)])
    at = [jnp.reshape((x + d) % NX, (1,)).astype(jnp.int32) for d in range(NX)]

    def send(block, d):
        return lax.ppermute(block, "x", [(i, (i + d) % NX) for i in range(NX)])

    (two,) = fold(at[2], own_q, (blocks,))
    (two,) = fold(at[2], own_q, (others,), (two,), packed=True)
    two = send(two, 2)
    (one,) = fold(at[1], own_q, (blocks, others), packed=True)
    one = send(one, 1)
    (three,) = fold(at[3], own_q, (blocks, others), packed=True)
    three = send(three, 3)
    (kept,) = fold(at[0], own_q, (blocks, others))
    mixed = call(finish_kernel, bf16(TOK, wo.shape[1]), kept, two, one, three, wo, flops=2 * TOK * 1024 * 1024)
    shares = lax.all_to_all(mixed.reshape(NY, rows, -1), "y", 0, 0, tiled=True)
    return call(sum_kernel, bf16(rows, dim), shares)


def solution(mesh):
    fine = Mesh(mesh.devices.reshape(NZ, NX, NC, NY), ("z", "x", "c", "y"))
    sp = ("z", "x", "c")
    tables = rotary_tables(NZ * NX * NC * TOK // GRID_W)

    def run(*args):
        return per_device(tables, *args)

    return jax.shard_map(
        run,
        mesh=fine,
        in_specs=(
            P(sp + ("y",), None),
            P(),
            P(None, "y"),
            P(None, "y"),
            P(None, "y"),
            P(),
            P(),
            P("y", None),
        ),
        out_specs=P(sp + ("y",), None),
        check_vma=False,
    )
```

```python
import math

import jax
import jax.numpy as jnp
import numpy as np
from jax import lax
from jax.experimental import pallas as pl
from jax.experimental.pallas import tpu as pltpu
from jax.sharding import Mesh, PartitionSpec as P


GRID_W = 64
EPS = 1e-06
BASE = 10000.0
HD = 128
TOK = 128
NZ, NX, NC, NY = 16, 4, 2, 4
KEY_SCALE, VALUE_SCALE = 2.0**11, 2.0**7
LROWS = 8
AROWS = HD + LROWS
PROWS = HD + LROWS
RINGS = [[i * NC + (i + g) % NC for i in range(NZ)] for g in range(NC)]
CHUNK = 512


def rotary_tables(grid_rows):
    axis_dim = HD // 2
    freq = np.power(np.float32(BASE), -np.arange(0, axis_dim, 2, dtype=np.float32) / np.float32(axis_dim))
    sign = np.tile(np.array([-1.0, 1.0]), axis_dim // 2)

    def half(count):
        angle = (np.arange(count, dtype=np.float32)[:, None] * freq[None, :].astype(np.float32)).astype(np.float64)
        angle = np.repeat(angle, 2, axis=1)
        return np.cos(angle), np.sin(angle) * sign

    row_cos, row_sin = half(grid_rows)
    col_cos, col_sin = half(GRID_W)
    pad_r, pad_c = np.ones_like(row_cos), np.ones_like(col_cos)
    rows = np.stack([np.concatenate([row_cos, pad_r], 1), np.concatenate([row_sin, pad_r], 1)])
    cols = np.stack([np.concatenate([pad_c, col_cos], 1), np.concatenate([pad_c, col_sin], 1)])
    return rows.astype(np.float32), cols.astype(np.float32)


VM = pl.BlockSpec(memory_space=pltpu.VMEM)


def call(kernel, shapes, *args, smem=0, flops=0, limit=24, alias=None):
    return pl.pallas_call(
        kernel,
        out_shape=shapes,
        in_specs=[pl.BlockSpec(memory_space=pltpu.SMEM)] * smem + [VM] * (len(args) - smem),
        out_specs=jax.tree.map(lambda s: VM, shapes),
        input_output_aliases=alias or {},
        cost_estimate=pl.CostEstimate(flops=flops, bytes_accessed=1 << 20, transcendentals=0),
        compiler_params=pltpu.CompilerParams(vmem_limit_bytes=limit << 20),
    )(*args)


def bf16(*shape):
    return jax.ShapeDtypeStruct(shape, jnp.bfloat16)


def f32(*shape):
    return jax.ShapeDtypeStruct(shape, jnp.float32)


def spread_kernel(tok_ref, out_ref, sems):
    copies = [pltpu.make_async_copy(tok_ref, out_ref.at[i], sems.at[i]) for i in range(NY)]
    for copy in copies:
        copy.start()
    for copy in copies:
        copy.wait()


def spread(array, count):
    return pl.pallas_call(
        spread_kernel,
        out_shape=jax.ShapeDtypeStruct((count,) + array.shape, array.dtype),
        in_specs=[VM],
        out_specs=pl.BlockSpec(memory_space=pltpu.HBM),
        scratch_shapes=[pltpu.SemaphoreType.DMA((count,))],
        name="spread",
    )(array)


def project_kernel(sp_ref, tok_ref, w_ref, vec_ref, rows_ref, cols_ref, q_ref, kv_ref, turned_ref, sems):
    x = tok_ref[...].astype(jnp.float32)
    dim = x.shape[1]
    wide_q = w_ref.shape[1] - 2 * HD
    query_gain, key_gain = vec_ref[:, dim : dim + HD], vec_ref[:, dim + HD :]
    normed = x * lax.rsqrt(jnp.mean(x * x, axis=-1, keepdims=True) + EPS) * vec_ref[:, :dim]
    normed = normed.astype(jnp.bfloat16)
    first = sp_ref[0] * (TOK // GRID_W)

    def table(i):
        parts = [rows_ref[i, pl.ds(first + r, 1), :] * cols_ref[i] for r in range(TOK // GRID_W)]
        return jnp.concatenate(parts, axis=0)

    cosine, sine = table(0), table(1)
    even = lax.broadcasted_iota(jnp.int32, (TOK, HD), 1) % 2 == 0

    def turn(projected, gain):
        wide = projected.astype(jnp.bfloat16).astype(jnp.float32)
        wide = wide * lax.rsqrt(jnp.mean(wide * wide, axis=-1, keepdims=True) + EPS) * gain
        swapped = jnp.where(even, pltpu.roll(wide, HD - 1, 1), pltpu.roll(wide, 1, 1))
        return wide * cosine + swapped * sine

    keys = jnp.dot(normed, w_ref[:, wide_q : wide_q + HD], preferred_element_type=jnp.float32)
    keys = turn(keys, key_gain).astype(jnp.bfloat16) * KEY_SCALE
    values = jnp.dot(normed, w_ref[:, wide_q + HD :], preferred_element_type=jnp.float32).T.astype(jnp.bfloat16) * VALUE_SCALE
    kv_ref[0] = keys
    kv_ref[1] = values
    queries = jnp.dot(normed, w_ref[:, :wide_q], preferred_element_type=jnp.float32)
    fold = HD ** (-0.5) * math.log2(math.e) / KEY_SCALE
    for h in range(queries.shape[1] // HD):
        turned = turn(queries[:, h * HD : (h + 1) * HD], query_gain) * fold
        turned_ref[:, h * TOK : (h + 1) * TOK] = turned.T.astype(jnp.bfloat16)
    copies = [pltpu.make_async_copy(turned_ref, q_ref.at[i], sems.at[i]) for i in range(NX)]
    for copy in copies:
        copy.start()
    for copy in copies:
        copy.wait()


def pack(total):
    below = total[HD:]
    high = below.astype(jnp.bfloat16).astype(jnp.float32)
    odd = lax.broadcasted_iota(jnp.int32, below.shape, 0) % 2 == 1
    return jnp.concatenate([total[:HD], jnp.where(odd, below - high, high)], axis=0).astype(jnp.bfloat16)


def unpack(packed):
    wide = packed.astype(jnp.float32)
    return jnp.concatenate([wide[:HD], wide[HD : HD + 1] + wide[HD + 1 : HD + 2]], axis=0)


def fold_kernel(steps, sets, resumed, packed, sp_ref, q_ref, *refs):
    tiles = len(steps)
    x = (sp_ref[0] // NC) % NX
    kv_refs, sum_refs, out_refs = refs[:sets], refs[sets : len(refs) - tiles], refs[len(refs) - tiles :]
    ones = jnp.full((LROWS, CHUNK), VALUE_SCALE, jnp.bfloat16)
    per = CHUNK // TOK
    keys, values = [], []
    for kv_ref in kv_refs:
        for j in range(0, kv_ref.shape[0], per):
            keys.append(jnp.concatenate([kv_ref[i, 0] for i in range(j, j + per)], axis=0))
            columns = jnp.concatenate([kv_ref[i, 1] for i in range(j, j + per)], axis=1)
            values.append(jnp.concatenate([columns, ones], axis=0))
    for t in range(tiles):
        q = q_ref[(x + steps[t]) % NX]
        total = sum_refs[t][...] if resumed else None
        for k, v in zip(keys, values):
            weights = jnp.exp2(jnp.dot(k, q, preferred_element_type=jnp.float32)).astype(jnp.bfloat16)
            part = jnp.dot(v, weights, preferred_element_type=jnp.float32)
            total = part if total is None else total + part
        out_refs[t][...] = pack(total) if packed else total


def fold(sp, steps, queries, blocks, sums=(), packed=False):
    tiles = len(steps)
    width = queries.shape[2]
    shape = tuple(bf16(PROWS, width) if packed else f32(AROWS, width) for _ in range(tiles))

    def kernel(*refs):
        fold_kernel(steps, len(blocks), len(sums) > 0, packed, *refs)

    flops = 4 * tiles * width * sum(b.shape[0] for b in blocks) * TOK * HD
    return call(kernel, shape, sp, queries, *blocks, *sums, smem=1, flops=flops)


def finish_kernel(own_ref, *refs):
    part_refs, w_ref, out_ref = refs[:-2], refs[-2], refs[-1]
    total = own_ref[: HD + 1]
    for part_ref in part_refs:
        total = total + unpack(part_ref[...])
    quotient = total[:HD] * (1.0 / total[HD : HD + 1])
    heads = [quotient[:, i : i + TOK].T.astype(jnp.bfloat16) for i in range(0, quotient.shape[1], TOK)]
    attended = jnp.concatenate(heads, axis=1)
    out_ref[...] = jnp.dot(attended, w_ref[...], preferred_element_type=jnp.float32).astype(jnp.bfloat16)


def sum_kernel(part_ref, out_ref):
    total = part_ref[0].astype(jnp.float32)
    for p in range(1, part_ref.shape[0]):
        total = total + part_ref[p].astype(jnp.float32)
    out_ref[...] = total.astype(out_ref.dtype)


def per_device(tables, tokens, norm_gain, wq, wk, wv, query_gain, key_gain, wo):
    z, x, c = (lax.axis_index(a) for a in ("z", "x", "c"))
    sp = jnp.reshape((z * NX + x) * NC + c, (1,)).astype(jnp.int32)
    rows, dim = tokens.shape
    width = wq.shape[1]
    copies = spread(tokens, NY)
    mine = lax.all_to_all(copies, "y", 0, 0, tiled=True).reshape(NY * rows, dim)
    weights = jnp.concatenate([wq, wk, wv], axis=1)
    gains = jnp.concatenate([norm_gain, query_gain, key_gain]).reshape(1, -1)
    q, kv = pl.pallas_call(
        project_kernel,
        out_shape=(bf16(NX, HD, width), bf16(2, TOK, HD)),
        in_specs=[pl.BlockSpec(memory_space=pltpu.SMEM)] + [VM] * 5,
        out_specs=(pl.BlockSpec(memory_space=pltpu.HBM), VM),
        scratch_shapes=[pltpu.VMEM((HD, width), jnp.bfloat16), pltpu.SemaphoreType.DMA((NX,))],
        name="project",
        cost_estimate=pl.CostEstimate(flops=2 * TOK * dim * (width + 2 * HD), bytes_accessed=1 << 20, transcendentals=0),
        compiler_params=pltpu.CompilerParams(vmem_limit_bytes=24 << 20),
    )(sp, mine, weights, gains, *tables)
    own_q = lax.all_to_all(q, "x", 0, 0, tiled=True)
    scaled = kv.astype(jnp.float16)
    gathered = lax.all_gather(scaled[None], ("z", "c"), axis_index_groups=RINGS, axis=0, tiled=True)
    blocks = gathered.astype(jnp.bfloat16)
    others = lax.ppermute(blocks, "c", [(0, 1), (1, 0)])

    def send(block, d):
        return lax.ppermute(block, "x", [(i, (i + d) % NX) for i in range(NX)])

    (two,) = fold(sp, (2,), own_q, (blocks,))
    (two,) = fold(sp, (2,), own_q, (others,), (two,), packed=True)
    two = send(two, 2)
    (one,) = fold(sp, (1,), own_q, (blocks, others), packed=True)
    one = send(one, 1)
    (three,) = fold(sp, (3,), own_q, (blocks, others), packed=True)
    three = send(three, 3)
    (kept,) = fold(sp, (0,), own_q, (blocks, others))
    mixed = call(finish_kernel, bf16(TOK, wo.shape[1]), kept, two, one, three, wo, flops=2 * TOK * 1024 * 1024)
    shares = lax.all_to_all(mixed.reshape(NY, rows, -1), "y", 0, 0, tiled=True)
    return call(sum_kernel, bf16(rows, dim), shares)


def solution(mesh):
    fine = Mesh(mesh.devices.reshape(NZ, NX, NC, NY), ("z", "x", "c", "y"))
    sp = ("z", "x", "c")
    tables = rotary_tables(NZ * NX * NC * TOK // GRID_W)

    def run(*args):
        return per_device(tables, *args)

    return jax.shard_map(
        run,
        mesh=fine,
        in_specs=(
            P(sp + ("y",), None),
            P(),
            P(None, "y"),
            P(None, "y"),
            P(None, "y"),
            P(),
            P(),
            P("y", None),
        ),
        out_specs=P(sp + ("y",), None),
        check_vma=False,
    )
```

```python
import math

import jax
import jax.numpy as jnp
import numpy as np
from jax import lax
from jax.experimental import pallas as pl
from jax.experimental.pallas import tpu as pltpu
from jax.sharding import Mesh, PartitionSpec as P


GRID_W = 64
EPS = 1e-06
BASE = 10000.0
HD = 128
TOK = 128
NZ, NX, NC, NY = 16, 4, 2, 4
KEY_SCALE, VALUE_SCALE = 2.0**11, 2.0**7
LROWS = 8
AROWS = HD + LROWS
PROWS = HD + LROWS
TURNS = ((1, 3), (2, 2), (3, 1))
RINGS = [[i * NC + (i + g) % NC for i in range(NZ)] for g in range(NC)]
CHUNK = 512


def rotary_tables(grid_rows):
    axis_dim = HD // 2
    freq = np.power(np.float32(BASE), -np.arange(0, axis_dim, 2, dtype=np.float32) / np.float32(axis_dim))
    sign = np.tile(np.array([-1.0, 1.0]), axis_dim // 2)

    def half(count):
        angle = (np.arange(count, dtype=np.float32)[:, None] * freq[None, :].astype(np.float32)).astype(np.float64)
        angle = np.repeat(angle, 2, axis=1)
        return np.cos(angle), np.sin(angle) * sign

    row_cos, row_sin = half(grid_rows)
    col_cos, col_sin = half(GRID_W)
    pad_r, pad_c = np.ones_like(row_cos), np.ones_like(col_cos)
    rows = np.stack([np.concatenate([row_cos, pad_r], 1), np.concatenate([row_sin, pad_r], 1)])
    cols = np.stack([np.concatenate([pad_c, col_cos], 1), np.concatenate([pad_c, col_sin], 1)])
    return rows.astype(np.float32), cols.astype(np.float32)


VM = pl.BlockSpec(memory_space=pltpu.VMEM)


def call(kernel, shapes, *args, smem=0, flops=0, limit=24, alias=None):
    return pl.pallas_call(
        kernel,
        out_shape=shapes,
        in_specs=[pl.BlockSpec(memory_space=pltpu.SMEM)] * smem + [VM] * (len(args) - smem),
        out_specs=jax.tree.map(lambda s: VM, shapes),
        input_output_aliases=alias or {},
        cost_estimate=pl.CostEstimate(flops=flops, bytes_accessed=1 << 20, transcendentals=0),
        compiler_params=pltpu.CompilerParams(vmem_limit_bytes=limit << 20),
    )(*args)


def bf16(*shape):
    return jax.ShapeDtypeStruct(shape, jnp.bfloat16)


def f32(*shape):
    return jax.ShapeDtypeStruct(shape, jnp.float32)


def spread_kernel(tok_ref, out_ref, sems):
    copies = [pltpu.make_async_copy(tok_ref, out_ref.at[i], sems.at[i]) for i in range(NY)]
    for copy in copies:
        copy.start()
    for copy in copies:
        copy.wait()


def spread(array, count):
    return pl.pallas_call(
        spread_kernel,
        out_shape=jax.ShapeDtypeStruct((count,) + array.shape, array.dtype),
        in_specs=[VM],
        out_specs=pl.BlockSpec(memory_space=pltpu.HBM),
        scratch_shapes=[pltpu.SemaphoreType.DMA((count,))],
        name="spread",
    )(array)


def project_kernel(sp_ref, tok_ref, w_ref, vec_ref, rows_ref, cols_ref, q_ref, kv_ref, turned_ref, sems):
    x = tok_ref[...].astype(jnp.float32)
    dim = x.shape[1]
    wide_q = w_ref.shape[1] - 2 * HD
    query_gain, key_gain = vec_ref[:, dim : dim + HD], vec_ref[:, dim + HD :]
    normed = x * lax.rsqrt(jnp.mean(x * x, axis=-1, keepdims=True) + EPS) * vec_ref[:, :dim]
    normed = normed.astype(jnp.bfloat16)
    first = sp_ref[0] * (TOK // GRID_W)

    def table(i):
        parts = [rows_ref[i, pl.ds(first + r, 1), :] * cols_ref[i] for r in range(TOK // GRID_W)]
        return jnp.concatenate(parts, axis=0)

    cosine, sine = table(0), table(1)
    even = lax.broadcasted_iota(jnp.int32, (TOK, HD), 1) % 2 == 0

    def turn(projected, gain):
        wide = projected.astype(jnp.bfloat16).astype(jnp.float32)
        wide = wide * lax.rsqrt(jnp.mean(wide * wide, axis=-1, keepdims=True) + EPS) * gain
        swapped = jnp.where(even, pltpu.roll(wide, HD - 1, 1), pltpu.roll(wide, 1, 1))
        return wide * cosine + swapped * sine

    keys = jnp.dot(normed, w_ref[:, wide_q : wide_q + HD], preferred_element_type=jnp.float32)
    keys = turn(keys, key_gain).astype(jnp.bfloat16) * KEY_SCALE
    values = jnp.dot(normed, w_ref[:, wide_q + HD :], preferred_element_type=jnp.float32).T.astype(jnp.bfloat16) * VALUE_SCALE
    kv_ref[0] = keys
    kv_ref[1] = values
    queries = jnp.dot(normed, w_ref[:, :wide_q], preferred_element_type=jnp.float32)
    fold = HD ** (-0.5) * math.log2(math.e) / KEY_SCALE
    for h in range(queries.shape[1] // HD):
        turned = turn(queries[:, h * HD : (h + 1) * HD], query_gain) * fold
        turned_ref[:, h * TOK : (h + 1) * TOK] = turned.T.astype(jnp.bfloat16)
    copies = [pltpu.make_async_copy(turned_ref, q_ref.at[i], sems.at[i]) for i in range(NX)]
    for copy in copies:
        copy.start()
    for copy in copies:
        copy.wait()


def pack(total):
    below = total[HD:]
    high = below.astype(jnp.bfloat16).astype(jnp.float32)
    odd = lax.broadcasted_iota(jnp.int32, below.shape, 0) % 2 == 1
    return jnp.concatenate([total[:HD], jnp.where(odd, below - high, high)], axis=0).astype(jnp.bfloat16)


def unpack(packed):
    wide = packed.astype(jnp.float32)
    return jnp.concatenate([wide[:HD], wide[HD : HD + 1] + wide[HD + 1 : HD + 2]], axis=0)


def fold_kernel(steps, sets, resumed, packed, sp_ref, q_ref, *refs):
    place = (sp_ref[0] // NC + steps[0] + sp_ref[0] % NC * (steps[1] - steps[0])) % NX
    kv_refs, sum_ref, out_ref = refs[:sets], refs[sets], refs[-1]
    ones = jnp.full((LROWS, CHUNK), VALUE_SCALE, jnp.bfloat16)
    per = CHUNK // TOK
    keys, values = [], []
    for kv_ref in kv_refs:
        for j in range(0, kv_ref.shape[0], per):
            keys.append(jnp.concatenate([kv_ref[i, 0] for i in range(j, j + per)], axis=0))
            columns = jnp.concatenate([kv_ref[i, 1] for i in range(j, j + per)], axis=1)
            values.append(jnp.concatenate([columns, ones], axis=0))
    q = q_ref[place]
    total = sum_ref[...] if resumed else None
    for k, v in zip(keys, values):
        weights = jnp.exp2(jnp.dot(k, q, preferred_element_type=jnp.float32)).astype(jnp.bfloat16)
        part = jnp.dot(v, weights, preferred_element_type=jnp.float32)
        total = part if total is None else total + part
    out_ref[...] = pack(total) if packed else total


def fold(sp, steps, queries, blocks, sums=(), packed=False):
    width = queries.shape[2]
    shape = bf16(PROWS, width) if packed else f32(AROWS, width)

    def kernel(*refs):
        fold_kernel(steps, len(blocks), len(sums) > 0, packed, *refs)

    flops = 4 * width * sum(b.shape[0] for b in blocks) * TOK * HD
    return call(kernel, shape, sp, queries, *blocks, *sums, smem=1, flops=flops)


def finish_kernel(own_ref, *refs):
    part_refs, w_ref, out_ref = refs[:-2], refs[-2], refs[-1]
    total = own_ref[: HD + 1]
    for part_ref in part_refs:
        total = total + unpack(part_ref[...])
    quotient = total[:HD] * (1.0 / total[HD : HD + 1])
    heads = [quotient[:, i : i + TOK].T.astype(jnp.bfloat16) for i in range(0, quotient.shape[1], TOK)]
    attended = jnp.concatenate(heads, axis=1)
    out_ref[...] = jnp.dot(attended, w_ref[...], preferred_element_type=jnp.float32).astype(jnp.bfloat16)


def sum_kernel(part_ref, out_ref):
    total = part_ref[0].astype(jnp.float32)
    for p in range(1, part_ref.shape[0]):
        total = total + part_ref[p].astype(jnp.float32)
    out_ref[...] = total.astype(out_ref.dtype)


def per_device(tables, tokens, norm_gain, wq, wk, wv, query_gain, key_gain, wo):
    z, x, c = (lax.axis_index(a) for a in ("z", "x", "c"))
    sp = jnp.reshape((z * NX + x) * NC + c, (1,)).astype(jnp.int32)
    rows, dim = tokens.shape
    width = wq.shape[1]
    copies = spread(tokens, NY)
    mine = lax.all_to_all(copies, "y", 0, 0, tiled=True).reshape(NY * rows, dim)
    weights = jnp.concatenate([wq, wk, wv], axis=1)
    gains = jnp.concatenate([norm_gain, query_gain, key_gain]).reshape(1, -1)
    q, kv = pl.pallas_call(
        project_kernel,
        out_shape=(bf16(NX, HD, width), bf16(2, TOK, HD)),
        in_specs=[pl.BlockSpec(memory_space=pltpu.SMEM)] + [VM] * 5,
        out_specs=(pl.BlockSpec(memory_space=pltpu.HBM), VM),
        scratch_shapes=[pltpu.VMEM((HD, width), jnp.bfloat16), pltpu.SemaphoreType.DMA((NX,))],
        name="project",
        cost_estimate=pl.CostEstimate(flops=2 * TOK * dim * (width + 2 * HD), bytes_accessed=1 << 20, transcendentals=0),
        compiler_params=pltpu.CompilerParams(vmem_limit_bytes=24 << 20),
    )(sp, mine, weights, gains, *tables)
    own_q = lax.all_to_all(q, "x", 0, 0, tiled=True)
    scaled = kv.astype(jnp.float16)
    gathered = lax.all_gather(scaled[None], ("z", "c"), axis_index_groups=RINGS, axis=0, tiled=True)
    blocks = gathered.astype(jnp.bfloat16)
    others = lax.ppermute(blocks, "c", [(0, 1), (1, 0)])

    def send(block, slot):
        pairs = [(i * NC + j, (i + TURNS[slot][j]) % NX * NC + j) for i in range(NX) for j in range(NC)]
        return lax.ppermute(block, ("x", "c"), pairs)

    begun = fold(sp, TURNS[0], own_q, (blocks,))
    sums = fold(sp, TURNS[0], own_q, (others,), (begun,), packed=True)
    came = [send(sums, 0)]
    for slot in (1, 2):
        sums = fold(sp, TURNS[slot], own_q, (blocks, others), packed=True)
        came.append(send(sums, slot))
    kept = fold(sp, (0, 0), own_q, (blocks, others))
    mixed = call(finish_kernel, bf16(TOK, wo.shape[1]), kept, *came, wo, flops=2 * TOK * 1024 * 1024)
    shares = lax.all_to_all(mixed.reshape(NY, rows, -1), "y", 0, 0, tiled=True)
    return call(sum_kernel, bf16(rows, dim), shares)


def solution(mesh):
    fine = Mesh(mesh.devices.reshape(NZ, NX, NC, NY), ("z", "x", "c", "y"))
    sp = ("z", "x", "c")
    tables = rotary_tables(NZ * NX * NC * TOK // GRID_W)

    def run(*args):
        return per_device(tables, *args)

    return jax.shard_map(
        run,
        mesh=fine,
        in_specs=(
            P(sp + ("y",), None),
            P(),
            P(None, "y"),
            P(None, "y"),
            P(None, "y"),
            P(),
            P(),
            P("y", None),
        ),
        out_specs=P(sp + ("y",), None),
        check_vma=False,
    )
```

```python
import math

import jax
import jax.numpy as jnp
import numpy as np
from jax import lax
from jax.experimental import pallas as pl
from jax.experimental.pallas import tpu as pltpu
from jax.sharding import Mesh, PartitionSpec as P


GRID_W = 64
EPS = 1e-06
BASE = 10000.0
HD = 128
TOK = 128
NZ, NX, NC, NY = 16, 4, 2, 4
KEY_SCALE, VALUE_SCALE = 2.0**11, 2.0**7
LROWS = 8
AROWS = HD + LROWS
PROWS = HD + LROWS
TURNS = ((1, 3), (2, 2), (3, 1))
RINGS = [[i * NC + (i + g) % NC for i in range(NZ)] for g in range(NC)]
CHUNK = 1024


def rotary_tables(grid_rows):
    axis_dim = HD // 2
    freq = np.power(np.float32(BASE), -np.arange(0, axis_dim, 2, dtype=np.float32) / np.float32(axis_dim))
    sign = np.tile(np.array([-1.0, 1.0]), axis_dim // 2)

    def half(count):
        angle = (np.arange(count, dtype=np.float32)[:, None] * freq[None, :].astype(np.float32)).astype(np.float64)
        angle = np.repeat(angle, 2, axis=1)
        return np.cos(angle), np.sin(angle) * sign

    row_cos, row_sin = half(grid_rows)
    col_cos, col_sin = half(GRID_W)
    pad_r, pad_c = np.ones_like(row_cos), np.ones_like(col_cos)
    rows = np.stack([np.concatenate([row_cos, pad_r], 1), np.concatenate([row_sin, pad_r], 1)])
    cols = np.stack([np.concatenate([pad_c, col_cos], 1), np.concatenate([pad_c, col_sin], 1)])
    return rows.astype(np.float32), cols.astype(np.float32)


VM = pl.BlockSpec(memory_space=pltpu.VMEM)


def call(kernel, shapes, *args, smem=0, flops=0, limit=24, alias=None):
    return pl.pallas_call(
        kernel,
        out_shape=shapes,
        in_specs=[pl.BlockSpec(memory_space=pltpu.SMEM)] * smem + [VM] * (len(args) - smem),
        out_specs=jax.tree.map(lambda s: VM, shapes),
        input_output_aliases=alias or {},
        cost_estimate=pl.CostEstimate(flops=flops, bytes_accessed=1 << 20, transcendentals=0),
        compiler_params=pltpu.CompilerParams(vmem_limit_bytes=limit << 20),
    )(*args)


def bf16(*shape):
    return jax.ShapeDtypeStruct(shape, jnp.bfloat16)


def f32(*shape):
    return jax.ShapeDtypeStruct(shape, jnp.float32)


def spread_kernel(tok_ref, out_ref, sems):
    copies = [pltpu.make_async_copy(tok_ref, out_ref.at[i], sems.at[i]) for i in range(NY)]
    for copy in copies:
        copy.start()
    for copy in copies:
        copy.wait()


def spread(array, count):
    return pl.pallas_call(
        spread_kernel,
        out_shape=jax.ShapeDtypeStruct((count,) + array.shape, array.dtype),
        in_specs=[VM],
        out_specs=pl.BlockSpec(memory_space=pltpu.HBM),
        scratch_shapes=[pltpu.SemaphoreType.DMA((count,))],
        name="spread",
    )(array)


def project_kernel(sp_ref, tok_ref, w_ref, vec_ref, rows_ref, cols_ref, q_ref, kv_ref):
    x = tok_ref[...].astype(jnp.float32)
    dim = x.shape[1]
    wide_q = w_ref.shape[1] - 2 * HD
    query_gain, key_gain = vec_ref[:, dim : dim + HD], vec_ref[:, dim + HD :]
    normed = x * lax.rsqrt(jnp.mean(x * x, axis=-1, keepdims=True) + EPS) * vec_ref[:, :dim]
    normed = normed.astype(jnp.bfloat16)
    first = sp_ref[0] * (TOK // GRID_W)

    def table(i):
        parts = [rows_ref[i, pl.ds(first + r, 1), :] * cols_ref[i] for r in range(TOK // GRID_W)]
        return jnp.concatenate(parts, axis=0)

    cosine, sine = table(0), table(1)
    even = lax.broadcasted_iota(jnp.int32, (TOK, HD), 1) % 2 == 0

    def turn(projected, gain):
        wide = projected.astype(jnp.bfloat16).astype(jnp.float32)
        wide = wide * lax.rsqrt(jnp.mean(wide * wide, axis=-1, keepdims=True) + EPS) * gain
        swapped = jnp.where(even, pltpu.roll(wide, HD - 1, 1), pltpu.roll(wide, 1, 1))
        return wide * cosine + swapped * sine

    keys = jnp.dot(normed, w_ref[:, wide_q : wide_q + HD], preferred_element_type=jnp.float32)
    keys = turn(keys, key_gain).astype(jnp.bfloat16) * KEY_SCALE
    values = jnp.dot(normed, w_ref[:, wide_q + HD :], preferred_element_type=jnp.float32).T.astype(jnp.bfloat16) * VALUE_SCALE
    kv_ref[0] = keys
    kv_ref[1] = values
    queries = jnp.dot(normed, w_ref[:, :wide_q], preferred_element_type=jnp.float32)
    fold = HD ** (-0.5) * math.log2(math.e) / KEY_SCALE
    for h in range(queries.shape[1] // HD):
        turned = turn(queries[:, h * HD : (h + 1) * HD], query_gain) * fold
        q_ref[:, h * TOK : (h + 1) * TOK] = turned.T.astype(jnp.bfloat16)


def pack(total):
    below = total[HD:]
    high = below.astype(jnp.bfloat16).astype(jnp.float32)
    odd = lax.broadcasted_iota(jnp.int32, below.shape, 0) % 2 == 1
    return jnp.concatenate([total[:HD], jnp.where(odd, below - high, high)], axis=0).astype(jnp.bfloat16)


def unpack(packed):
    wide = packed.astype(jnp.float32)
    return jnp.concatenate([wide[:HD], wide[HD : HD + 1] + wide[HD + 1 : HD + 2]], axis=0)


def fold_kernel(steps, sets, resumed, packed, sp_ref, q_ref, *refs):
    place = (sp_ref[0] // NC + steps[0] + sp_ref[0] % NC * (steps[1] - steps[0])) % NX
    kv_refs, sum_ref, out_ref = refs[:sets], refs[sets], refs[-1]
    ones = jnp.full((LROWS, CHUNK), VALUE_SCALE, jnp.bfloat16)
    per = CHUNK // TOK
    keys, values = [], []
    for kv_ref in kv_refs:
        for j in range(0, kv_ref.shape[0], per):
            keys.append(jnp.concatenate([kv_ref[i, 0] for i in range(j, j + per)], axis=0))
            columns = jnp.concatenate([kv_ref[i, 1] for i in range(j, j + per)], axis=1)
            values.append(jnp.concatenate([columns, ones], axis=0))
    q = q_ref[place]
    total = sum_ref[...] if resumed else None
    for k, v in zip(keys, values):
        weights = jnp.exp2(jnp.dot(k, q, preferred_element_type=jnp.float32)).astype(jnp.bfloat16)
        part = jnp.dot(v, weights, preferred_element_type=jnp.float32)
        total = part if total is None else total + part
    out_ref[...] = pack(total) if packed else total


def fold(sp, steps, queries, blocks, sums=(), packed=False):
    width = queries.shape[2]
    shape = bf16(PROWS, width) if packed else f32(AROWS, width)

    def kernel(*refs):
        fold_kernel(steps, len(blocks), len(sums) > 0, packed, *refs)

    flops = 4 * width * sum(b.shape[0] for b in blocks) * TOK * HD
    return call(kernel, shape, sp, queries, *blocks, *sums, smem=1, flops=flops)


def finish_kernel(own_ref, *refs):
    part_refs, w_ref, out_ref = refs[:-2], refs[-2], refs[-1]
    total = own_ref[: HD + 1]
    for part_ref in part_refs:
        total = total + unpack(part_ref[...])
    quotient = total[:HD] * (1.0 / total[HD : HD + 1])
    heads = [quotient[:, i : i + TOK].T.astype(jnp.bfloat16) for i in range(0, quotient.shape[1], TOK)]
    attended = jnp.concatenate(heads, axis=1)
    out_ref[...] = jnp.dot(attended, w_ref[...], preferred_element_type=jnp.float32).astype(jnp.bfloat16)


def sum_kernel(part_ref, out_ref):
    total = part_ref[0].astype(jnp.float32)
    for p in range(1, part_ref.shape[0]):
        total = total + part_ref[p].astype(jnp.float32)
    out_ref[...] = total.astype(out_ref.dtype)


def per_device(tables, tokens, norm_gain, wq, wk, wv, query_gain, key_gain, wo):
    z, x, c = (lax.axis_index(a) for a in ("z", "x", "c"))
    sp = jnp.reshape((z * NX + x) * NC + c, (1,)).astype(jnp.int32)
    rows, dim = tokens.shape
    width = wq.shape[1]
    copies = spread(tokens, NY)
    mine = lax.all_to_all(copies, "y", 0, 0, tiled=True).reshape(NY * rows, dim)
    weights = jnp.concatenate([wq, wk, wv], axis=1)
    gains = jnp.concatenate([norm_gain, query_gain, key_gain]).reshape(1, -1)
    q, kv = pl.pallas_call(
        project_kernel,
        out_shape=(bf16(HD, width), bf16(2, TOK, HD)),
        in_specs=[pl.BlockSpec(memory_space=pltpu.SMEM)] + [VM] * 5,
        out_specs=(VM, VM),
        name="project",
        cost_estimate=pl.CostEstimate(flops=2 * TOK * dim * (width + 2 * HD), bytes_accessed=1 << 20, transcendentals=0),
        compiler_params=pltpu.CompilerParams(vmem_limit_bytes=24 << 20),
    )(sp, mine, weights, gains, *tables)
    own_q = lax.all_to_all(jnp.broadcast_to(q[None], (NX,) + q.shape), "x", 0, 0, tiled=True)
    scaled = kv.astype(jnp.float16)
    gathered = lax.all_gather(scaled[None], ("z", "c"), axis_index_groups=RINGS, axis=0, tiled=True)
    blocks = gathered.astype(jnp.bfloat16)
    others = lax.ppermute(blocks, "c", [(0, 1), (1, 0)])

    def send(block, slot):
        pairs = [(i * NC + j, (i + TURNS[slot][j]) % NX * NC + j) for i in range(NX) for j in range(NC)]
        return lax.ppermute(block, ("x", "c"), pairs)

    begun = fold(sp, TURNS[0], own_q, (blocks,))
    sums = fold(sp, TURNS[0], own_q, (others,), (begun,), packed=True)
    came = [send(sums, 0)]
    for slot in (1, 2):
        sums = fold(sp, TURNS[slot], own_q, (blocks, others), packed=True)
        came.append(send(sums, slot))
    kept = fold(sp, (0, 0), own_q, (blocks, others))
    mixed = call(finish_kernel, bf16(TOK, wo.shape[1]), kept, *came, wo, flops=2 * TOK * 1024 * 1024)
    shares = lax.all_to_all(mixed.reshape(NY, rows, -1), "y", 0, 0, tiled=True)
    return call(sum_kernel, bf16(rows, dim), shares)


def solution(mesh):
    fine = Mesh(mesh.devices.reshape(NZ, NX, NC, NY), ("z", "x", "c", "y"))
    sp = ("z", "x", "c")
    tables = rotary_tables(NZ * NX * NC * TOK // GRID_W)

    def run(*args):
        return per_device(tables, *args)

    return jax.shard_map(
        run,
        mesh=fine,
        in_specs=(
            P(sp + ("y",), None),
            P(),
            P(None, "y"),
            P(None, "y"),
            P(None, "y"),
            P(),
            P(),
            P("y", None),
        ),
        out_specs=P(sp + ("y",), None),
        check_vma=False,
    )
```
